32 devices in a mesh: kv: 8 (over z, y), tp: 4 (over x, core).
Axes of the slice: x: 2, y: 2, z: 4, core: 2. Of those that a mesh axis runs over, the one named last changes fastest.
Arguments:
- layer_input: bfloat16 [4, 4096, 2048], P(None, 'kv', 'tp'), may hold values from -0.119628906 to 0.119628906
- queries: bfloat16 [4, 4096, 2048], P(None, 'kv', 'tp'), may hold values from -3.5 to 3.5
- keys: bfloat16 [4, 4096, 2048], P(None, 'kv', 'tp'), may hold values from -3.5 to 3.5
- values: bfloat16 [4, 4096, 2048], P(None, 'kv', 'tp'), may hold values from -5 to 5
- outputs: bfloat16 [4, 4096, 2048], P(None, 'kv', 'tp'), may hold values from -1.5 to 1.5
- d_out: bfloat16 [4, 4096, 2048], P(None, 'kv', 'tp'), may hold values from -30 to 30
- log_sums: float32 [4, 4096, 16], P(None, 'kv', 'tp'), may hold values from 6 to 8
- chosen: int32 [4, 64, 12], P(None, 'kv'), may hold values from -1 to 63, as said below
Outputs:
- d_queries: bfloat16 [4, 4096, 2048], P(None, 'kv', 'tp')
- d_keys: bfloat16 [4, 4096, 2048], P(None, 'kv', 'tp')
- d_values: bfloat16 [4, 4096, 2048], P(None, 'kv', 'tp')
- d_weight: float32 [2048, 2048], P('kv', 'tp')
The draws below stay inside these ranges and needn't reach their ends.
Inputs may be any that keep to these rules, and one draw needn't show every extreme that they name: Row chosen[s, b] names key blocks of sequence s for query block b: its first entry is b itself, the others are distinct blocks with smaller indices, either on the same device as b or on earlier devices; -1 marks unused slots, which come last. Over all sequences, the blocks of one device that query blocks of other devices name are at most 2, and in every draw some devices' are exactly 2.
All inputs are finite; a program needn't handle non-finite values.
Results may differ from the reference program's by a relative error of at most 0.0055.
Values may be sent and summed in bfloat16 or wider, within the bound.
A program may use at most 256 MiB of HBM per device.

```python
import jax
import jax.numpy as jnp
from jax import lax

D = 2048
HEADS = 16
DH = 128
HD = 2048
BLK = 64
SEL = 12
CAP = 2
SEQS = 4
TOK_DEV = 512
NPOS = 4096
NBLK = 64


def draw_chosen(key, part):
    local_blocks = TOK_DEV // BLK
    devices = NBLK // local_blocks
    own_blocks = SEQS * local_blocks
    pool_size = local_blocks + devices * CAP
    publish_key = jax.random.fold_in(key, 11)
    choose_key = jax.random.fold_in(key, 12)
    ranking = jax.random.randint(publish_key, (devices, own_blocks), 0, 4096) * own_blocks
    ranking = ranking + jnp.arange(own_blocks, dtype=jnp.int32)[None, :]
    published = jnp.argsort(-ranking, axis=1)[:, :CAP].astype(jnp.int32)
    owner_ids = jnp.arange(devices, dtype=jnp.int32)
    remote_seq = (published // local_blocks).reshape(devices * CAP)
    remote_block = (owner_ids[:, None] * local_blocks + published % local_blocks).reshape(devices * CAP)
    remote_owner = jnp.repeat(owner_ids, CAP)
    sequence_ids = jnp.arange(SEQS, dtype=jnp.int32)[:, None, None]
    query_block = jnp.arange(NBLK, dtype=jnp.int32)[None, :, None]
    query_device = query_block // local_blocks
    query_local = query_block % local_blocks
    local_index = jnp.arange(local_blocks, dtype=jnp.int32)[None, None, :]
    local_extent = (SEQS, NBLK, local_blocks)
    remote_extent = (SEQS, NBLK, devices * CAP)
    local_block = jnp.broadcast_to(query_device * local_blocks + local_index, local_extent)
    local_ok = jnp.broadcast_to(local_index <= query_local, local_extent)
    local_level = jnp.broadcast_to((local_index == query_local).astype(jnp.int32) * 4, local_extent)
    remote_ok = (remote_owner[None, None, :] < query_device) & (remote_seq[None, None, :] == sequence_ids)
    nearby = (remote_owner[None, None, :] == query_device - 1) | (remote_owner[None, None, :] == query_device - devices // 2)
    remote_level = jnp.broadcast_to(nearby.astype(jnp.int32) * 2, remote_extent)
    blocks = jnp.concatenate([local_block, jnp.broadcast_to(remote_block[None, None, :], remote_extent)], axis=2)
    usable = jnp.concatenate([local_ok, jnp.broadcast_to(remote_ok, remote_extent)], axis=2)
    levels = jnp.concatenate([local_level, remote_level], axis=2)
    slot_ids = jnp.arange(pool_size, dtype=jnp.int32)
    jitter = jax.random.randint(choose_key, (SEQS, NBLK, pool_size), 0, 4096)
    scores = (levels * 4096 + jitter) * pool_size + slot_ids
    scores = jnp.where(usable, scores, -1 - slot_ids)
    ranked = jnp.argsort(-scores, axis=2)[:, :, :SEL]
    top_scores = jnp.take_along_axis(scores, ranked, axis=2)
    picked = jnp.take_along_axis(blocks, ranked, axis=2)
    return jnp.where(top_scores >= 0, picked, -1).astype(jnp.int32)


def spiked(values, key, source, target, shards_of, factor):
    owner, partner = [(jnp.arange(values.shape[axis_at]) // (values.shape[axis_at] // shards_of)).reshape([-1 if axis == axis_at else 1 for axis in range(values.ndim)]) for axis_at in (source, target)]
    chosen = jax.random.permutation(key, shards_of)[partner]
    strong = (owner == chosen) | (owner == (partner + shards_of // 2) % shards_of)
    return jnp.where(strong, factor * values, values)


def block_scale(stream_key, shape, shards, smallest, largest):
    gain, own = 1.0, jax.random.fold_in(stream_key, 6)
    for position, blocks in shards:
        draws = jnp.exp(jax.random.uniform(jax.random.fold_in(own, position), (blocks,), jnp.float32, smallest / len(shards), largest / len(shards)))
        gain = gain * jnp.repeat(draws, shape[position] // blocks).reshape([-1 if axis == position else 1 for axis in range(len(shape))])
    return gain


def normal_values(own_key, shape, scale, reach, shards=(), kind=jnp.bfloat16):
    array = scale * jax.random.normal(own_key, shape, jnp.float32)
    if shards:
        array = array * block_scale(own_key, shape, shards, -0.22, 0.18)
    return jnp.clip(array, -reach, reach).astype(kind)


def bell_draw_with(stream_key, shape, width, reach, cuts, heavy, kind=jnp.bfloat16):
    result = width * jax.random.normal(stream_key, shape, jnp.float32)
    if cuts:
        result = result * block_scale(stream_key, shape, cuts, -0.22, 0.18)
    return jnp.clip(spiked(result, jax.random.fold_in(stream_key, 3), *heavy), -reach, reach).astype(kind)


def setup_inputs(seed: int = 0) -> dict:
    seeds = jax.random.split(jax.random.key(seed), 9)
    layer_input = bell_draw_with(seeds[0], (SEQS, NPOS, D), 0.02, 0.119628906, ((1, 8), (2, 4)), (1, 2, 8, 2.0))
    queries = normal_values(seeds[1], (SEQS, NPOS, HD), 0.7, 3.5, ((1, 8), (2, 4)))
    keys = normal_values(seeds[2], (SEQS, NPOS, HD), 0.7, 3.5, ((1, 8), (2, 4)))
    values = normal_values(seeds[3], (SEQS, NPOS, HD), 1.0, 5.0, ((1, 8), (2, 4)))
    outputs = normal_values(seeds[4], (SEQS, NPOS, HD), 0.25, 1.5, ((1, 8), (2, 4)))
    d_out = normal_values(seeds[5], (SEQS, NPOS, HD), 6.0, 30.0, ((1, 8), (2, 4)))
    log_sums = jnp.clip(6.0 + 2.0 * jax.random.uniform(seeds[6], (SEQS, NPOS, HEADS), jnp.float32) ** block_scale(seeds[6], (SEQS, NPOS, HEADS), ((1, 8), (2, 4)), -0.2, 0.2), 6.0, 8.0)
    chosen = draw_chosen(jax.random.fold_in(seeds[8], 71), 0)
    return dict(layer_input=layer_input, queries=queries, keys=keys, values=values, outputs=outputs, d_out=d_out, log_sums=log_sums, chosen=chosen)


def one_sequence(bundle):
    queries, keys, values, outputs, d_out, log_sums, chosen = bundle
    inverse_root = DH ** -0.5
    query_blocks = queries.reshape(NBLK, BLK, HEADS, DH)
    key_blocks = keys.reshape(NBLK, BLK, HEADS, DH)
    value_blocks = values.reshape(NBLK, BLK, HEADS, DH)
    cotangent = d_out.reshape(NBLK, BLK, HEADS, DH)
    product = d_out.astype(jnp.float32) * outputs.astype(jnp.float32)
    deltas = jnp.sum(product.reshape(NBLK, BLK, HEADS, DH), axis=3)
    log_blocks = log_sums.reshape(NBLK, BLK, HEADS)
    offsets = jnp.arange(BLK, dtype=jnp.int32)

    def advance(totals, block_index):
        key_total, value_total = totals
        picked = chosen[block_index]
        in_use = picked >= 0
        clamped = jnp.maximum(picked, 0).astype(jnp.int32)
        key_picked = key_blocks[clamped].astype(jnp.float32)
        value_picked = value_blocks[clamped].astype(jnp.float32)
        key_place = clamped[:, None] * BLK + offsets[None, :]
        query_place = block_index * BLK + offsets
        visible = in_use[None, :, None] & (key_place[None, :, :] <= query_place[:, None, None])
        query_rows = query_blocks[block_index].astype(jnp.float32)
        grad_rows = cotangent[block_index].astype(jnp.float32)
        scores = jnp.einsum('qhd,ekhd->hqek', query_rows, key_picked) * inverse_root
        log_shift = log_blocks[block_index].T[:, :, None, None]
        prob_full = jnp.where(visible[None], jnp.exp(scores - log_shift), 0.0)
        prob_grad = jnp.einsum('qhd,ekhd->hqek', grad_rows, value_picked)
        score_grad = prob_full * (prob_grad - deltas[block_index].T[:, :, None, None])
        prob_low = lax.optimization_barrier(prob_full.astype(jnp.bfloat16)).astype(jnp.float32)
        score_low = lax.optimization_barrier(score_grad.astype(jnp.bfloat16)).astype(jnp.float32)
        grad_query = jnp.einsum('hqek,ekhd->qhd', score_low, key_picked) * inverse_root
        grad_key = jnp.einsum('hqek,qhd->ekhd', score_low, query_rows) * inverse_root
        grad_value = jnp.einsum('hqek,qhd->ekhd', prob_low, grad_rows)
        weight = in_use.astype(jnp.float32)[:, None, None, None]
        key_total = key_total.at[clamped].add(grad_key * weight)
        value_total = value_total.at[clamped].add(grad_value * weight)
        return (key_total, value_total), grad_query.astype(jnp.bfloat16)

    zeroed = jnp.zeros((NBLK, BLK, HEADS, DH), jnp.float32)
    totals, grad_query = lax.scan(advance, (zeroed, zeroed), jnp.arange(NBLK, dtype=jnp.int32))
    key_total, value_total = totals
    d_queries = grad_query.reshape(NPOS, HEADS * DH)
    d_keys = key_total.astype(jnp.bfloat16).reshape(NPOS, HEADS * DH)
    d_values = value_total.astype(jnp.bfloat16).reshape(NPOS, HEADS * DH)
    return d_queries, d_keys, d_values


def reference(layer_input, queries, keys, values, outputs, d_out, log_sums, chosen):
    d_queries, d_keys, d_values = lax.map(one_sequence, (queries, keys, values, outputs, d_out, log_sums, chosen))
    flat_input = layer_input.reshape(SEQS * NPOS, D)
    flat_values = d_values.reshape(SEQS * NPOS, HEADS * DH)
    d_weight = jnp.dot(flat_input.T, flat_values, preferred_element_type=jnp.float32)
    return d_queries, d_keys, d_values, d_weight
```

```python
import functools

import jax
import jax.numpy as jnp
from jax import lax
from jax.experimental import pallas as pl
from jax.experimental.pallas import tpu as pltpu
from jax.sharding import PartitionSpec as P

BLK = 64
CAP = 2
LOG2E = 1.4426950408889634
HIDDEN = 1e30
GROUP = 4
BATCH = 8
NONE = 1 << 20

NT = (((1,), (1,)), ((), ()))
NN = (((1,), (0,)), ((), ()))
TN = (((0,), (0,)), ((), ()))
bf16, f32, i32 = jnp.bfloat16, jnp.float32, jnp.int32


def dot(a, b, dims):
    return lax.dot_general(a, b, dims, preferred_element_type=f32)


def peer(index, axis="kv"):
    return dict(device_id={axis: index}, device_id_type=pl.DeviceIdType.MESH)


def remote(source, target, send, recv, index, axis="kv"):
    return pltpu.make_async_remote_copy(source, target, send, recv, **peer(index, axis))


def probabilities(k, v, q, g, shift, delta, scale, diagonal):
    prob = jnp.exp2(dot(k, q, NT) * (scale * LOG2E) - shift)
    if diagonal:
        rows = lax.broadcasted_iota(i32, prob.shape, 0)
        cols = lax.broadcasted_iota(i32, prob.shape, 1)
        prob = jnp.where(rows <= cols, prob, 0.0)
    dscore = prob * (dot(v, g, NT) - delta)
    return prob.astype(bf16), dscore.astype(bf16)


def kernel(
    devices, width, heads, scale,
    x_hbm, q_hbm, k_hbm, v_hbm, o_hbm, g_hbm, log_ref, chosen_ref,
    dq_hbm, dk_hbm, dv_hbm, dw_hbm,
    every, q, k, v, o, g, x, dq, dk, dv, delta, pool, dscore, terms, back_in, back_far, part, part_in,
    part_far, dw, table,
    load_sem, keep_sem, out_sem, every_send, every_recv, x_send, x_recv,
    own_send, own_recv, chain_send, chain_recv, pass_send, pass_recv,
    back_send, back_recv, home_send, home_recv, part_send, part_recv, sum_send, sum_recv,
):
    sequences, positions, channels = q.shape
    size = channels // heads
    blocks = positions // BLK
    outer = devices // 2
    me, lane = lax.axis_index("kv"), lax.axis_index("tp")
    a, b = me // 2, me % 2
    partner = a * 2 + (1 - b)
    core = lane // 2 * 2 + (1 - lane % 2)
    head = [slice(h * size, (h + 1) * size) for h in range(heads)]

    def load(j, s):
        source, target = ((k_hbm, k), (v_hbm, v), (q_hbm, q), (g_hbm, g), (o_hbm, o))[j]
        return pltpu.make_async_copy(source.at[s], target.at[s], load_sem.at[j, s])

    for j in range(5):
        for s in range(sequences):
            load(j, s).start()
    keep = pltpu.make_async_copy(x_hbm, x.at[lane], keep_sem)
    keep.start()

    barrier = pltpu.get_barrier_semaphore()
    for i in range(1, devices):
        pl.semaphore_signal(barrier, inc=1, **peer(lax.rem(me + i, devices)))
    for i in range(1, width):
        pl.semaphore_signal(barrier, inc=1, **peer(lax.rem(lane + i, width), "tp"))
    pl.semaphore_wait(barrier, devices + width - 2)

    asks = [
        remote(chosen_ref, every.at[me], every_send.at[i - 1], every_recv.at[i - 1], lax.rem(me + i, devices))
        for i in range(1, devices)
    ]
    for ask in asks:
        ask.start()
    x_far = [
        remote(x_hbm, x.at[lane], x_send.at[i - 1], x_recv.at[i - 1], lax.rem(lane + 2 * i, width), "tp")
        for i in range(1, width // 2)
    ]
    x_own = remote(x_hbm, x.at[lane], x_send.at[width - 2], x_recv.at[width - 2], core, "tp")
    x_onto = []
    for i in range(1, width // 2):
        origin = lax.rem(lane + width - 2 * i, width)
        at = width // 2 - 2 + i
        x_onto.append(remote(x.at[origin], x.at[origin], x_send.at[at], x_recv.at[at], core, "tp"))
    for copy in x_far + [x_own]:
        copy.start()
    every[pl.ds(me, 1)] = chosen_ref[...][None]

    seq_of = lax.broadcasted_iota(i32, (sequences,) + chosen_ref.shape[1:], 0)

    def named(owner):
        low = jnp.full(seq_of.shape, NONE, i32)
        for d in range(devices):
            local = every[d] - owner * blocks
            fits = (local >= 0) & (local < blocks) & (owner != d)
            low = jnp.where(fits, jnp.minimum(low, seq_of * blocks + local), low)
        first = jnp.min(low)
        rest = jnp.full(seq_of.shape, NONE, i32)
        for d in range(devices):
            local = every[d] - owner * blocks
            fits = (local >= 0) & (local < blocks) & (owner != d)
            value = seq_of * blocks + local
            rest = jnp.where(fits & (value != first), jnp.minimum(rest, value), rest)
        return first, jnp.min(rest)

    for ask in asks:
        ask.wait_recv()
    mine = named(me)
    for j in range(2):
        for s in range(sequences):
            load(j, s).wait()
    for n in range(CAP):
        block = jnp.where(mine[n] < NONE, mine[n], 0)
        s, place = lax.div(block, blocks), lax.rem(block, blocks)
        pool[me, 0, n] = k[s, place]
        pool[me, 1, n] = v[s, place]

    def own():
        return remote(pool.at[a * 2], pool.at[a * 2], own_send, own_recv, partner)

    def chain(r):
        at = pool.at[(a - r) * 2 + b]
        return remote(at, at, chain_send.at[r], chain_recv.at[r], (a + 1) * 2 + b)

    def arrive(r):
        at = pool.at[(a - r) * 2 + b]
        return remote(at, at, chain_send.at[r - 1], chain_recv.at[r - 1], partner)

    def onto(r, side):
        at = pool.at[(a - r) * 2 + side]
        return remote(at, at, pass_send.at[r - 1], pass_recv.at[r - 1], partner)

    @pl.when(b == 0)
    def _():
        own().start()

    @pl.when(a + 1 < outer)
    def _():
        chain(0).start()

    def relay(r):
        @pl.when(r <= a)
        def _():
            arrive(r).wait_recv()
            onto(r, b).start()

            @pl.when(a + 1 < outer)
            def _():
                chain(r).start()

    dscore[...] = jnp.zeros_like(dscore)

    @pl.loop(0, devices)
    def _(d):
        first, second = named(d)
        table[d * CAP] = jnp.where(d < me, first, NONE)
        table[d * CAP + 1] = jnp.where(d < me, second, NONE)

    spread = lax.broadcasted_iota(i32, (blocks, positions), 1) // BLK == lax.broadcasted_iota(
        i32, (blocks, positions), 0
    )

    def hide_row(asked, block):
        sees = jnp.max(jnp.where(asked == block, 1.0, 0.0), axis=1, keepdims=True)
        sees = jnp.where(spread, sees, 0.0)
        return (1.0 - jnp.sum(sees, axis=0, keepdims=True)) * HIDDEN

    chunk = GROUP * BLK

    @pl.loop(0, sequences)
    def _(s):
        for j in range(2, 5):
            load(j, s).wait()
        for r in range(1, outer):
            @pl.when(s == min(sequences - 1, 1 + (r - 1) * sequences // outer))
            def _(r=r):
                relay(r)
        asked = chosen_ref[s]
        hide = [hide_row(asked, me * blocks + i) for i in range(blocks)]
        for h in range(heads):
            product = g[s, :, head[h]].astype(f32) * o[s, :, head[h]].astype(f32)
            delta_row = jnp.sum(product.T, axis=0, keepdims=True)
            delta[s, h : h + 1] = delta_row
            log_row = log_ref[s, h : h + 1]
            for start in range(0, positions, chunk):
                keys, rest = slice(start // BLK, start // BLK + GROUP), slice(start, positions)
                shift = jnp.concatenate([
                    jnp.broadcast_to((log_row + hide[start // BLK + i])[:, rest], (BLK, positions - start))
                    for i in range(GROUP)
                ], axis=0)
                qq, gg = q[s, rest, head[h]], g[s, rest, head[h]]
                kk = k[s, keys, :, head[h]].reshape(chunk, size)
                vv = v[s, keys, :, head[h]].reshape(chunk, size)
                prob, dsc = probabilities(kk, vv, qq, gg, shift, delta_row[:, rest], scale, True)
                if start == 0:
                    dq[s, :, head[h]] = dot(dsc, kk, TN)
                else:
                    dq[s, rest, head[h]] += dot(dsc, kk, TN)
                tall = (GROUP, BLK, size)
                dk[s, keys, :, head[h]] = (dot(dsc, qq, NN) * scale).astype(bf16).reshape(tall)
                dv[s, keys, :, head[h]] = dot(prob, gg, NN).astype(bf16).reshape(tall)

    def far_terms(owner, at):
        for n in range(CAP):
            ident = table[owner * CAP + n]
            valid = ident < NONE
            ident = jnp.where(valid, ident, 0)
            s = lax.div(ident, blocks)
            block = jnp.where(valid, owner * blocks + lax.rem(ident, blocks), -2)
            hide = hide_row(chosen_ref[s], block)
            logs, deltas = log_ref[s], delta[s]
            for h in range(heads):
                qq, gg = q[s, :, head[h]], g[s, :, head[h]]
                prob, dsc = probabilities(
                    pool[owner, 0, n, :, head[h]], pool[owner, 1, n, :, head[h]], qq, gg,
                    logs[h : h + 1] + hide, deltas[h : h + 1], scale, False,
                )
                dscore[h, pl.ds(pl.multiple_of((at * CAP + n) * BLK, BLK), BLK)] = dsc
                terms[0, owner, n, :, head[h]] = dot(prob, gg, NN).astype(bf16)
                terms[1, owner, n, :, head[h]] = (dot(dsc, qq, NN) * scale).astype(bf16)

    def back(kind, r):
        return remote(
            terms.at[kind, (a - r) * 2 + (1 - b)], back_in.at[kind, r],
            back_send.at[kind, r], back_recv.at[kind, r], partner,
        )

    def home(kind, r):
        return remote(
            back_in.at[kind, r], back_far.at[kind, r - 1],
            home_send.at[kind, r - 1], home_recv.at[kind, r - 1], (a - r) * 2 + b,
        )

    def query_terms(low):
        owners = min(devices - low, BATCH)
        for h in range(heads):
            masked = []
            for s in range(sequences):
                rows = []
                for i in range(owners):
                    for n in range(CAP):
                        ident = table[(low + i) * CAP + n]
                        rows.append(jnp.where(
                            lax.div(ident, blocks) == s, pool[low + i, 0, n, :, head[h]], 0.0
                        ).astype(bf16))
                masked.append(jnp.concatenate(rows, axis=0))
            more = dot(dscore[h], jnp.concatenate(masked, axis=1), TN)
            for s in range(sequences):
                dq[s, :, head[h]] += more[:, s * size : (s + 1) * size]

    @pl.when(b == 1)
    def _():
        own().wait_recv()
        far_terms(a * 2, (a * 2) % BATCH)
        back(0, 0).start()

    @pl.loop(1, a + 1)
    def _(r):
        direct, passed = (a - r) * 2 + b, (a - r) * 2 + (1 - b)
        onto(r, 1 - b).wait_recv()
        far_terms(passed, passed % BATCH)
        back(0, r).start()
        far_terms(direct, direct % BATCH)

    @pl.loop(1 - b, a + 1)
    def _(r):
        back(1, r).start()

    for copy in x_far:
        copy.wait_recv()
    for copy in x_onto:
        copy.start()

    def homeward(kind):
        @pl.loop(1, a + 1)
        def _(r):
            back(kind, r).wait_recv()
            both = terms[kind, (a - r) * 2 + b].astype(f32) + back_in[kind, r].astype(f32)
            back_in[kind, r] = both.astype(bf16)
            home(kind, r).start()

    def settle(kind, rows):
        @pl.when(b == 0)
        def _():
            back(kind, 0).wait_recv()

        @pl.when(b == 1)
        def _():
            back_in[kind, 0] = jnp.zeros(back_in.shape[2:], bf16)

        summed = back_in[kind, 0].astype(f32)
        for r in range(1, outer):
            @pl.when(a + r < outer)
            def _(r=r):
                home(kind, r).wait_recv()

            @pl.when(a + r >= outer)
            def _(r=r):
                back_far[kind, r - 1] = jnp.zeros(back_far.shape[2:], bf16)

            summed += back_far[kind, r - 1].astype(f32)
        fresh = []
        for n in range(CAP):
            block = jnp.where(mine[n] < NONE, mine[n], 0)
            s, place = lax.div(block, blocks), lax.rem(block, blocks)
            fresh.append((rows[s, place].astype(f32) + summed[n]).astype(bf16))
        for s in range(sequences):
            for i in range(blocks):
                value = rows[s, i]
                for n in range(CAP):
                    value = jnp.where(mine[n] == s * blocks + i, fresh[n], value)
                rows[s, i] = value

    homeward(0)
    settle(0, dv)
    put_dv = pltpu.make_async_copy(dv, dv_hbm, out_sem.at[0])
    put_dv.start()

    keep.wait()
    x_own.wait_recv()
    for copy in x_onto:
        copy.wait_recv()
    per = outer // width
    rows_each = dw.shape[0]

    def share(i):
        place = lax.rem(a // per + 1 + i // per, width) * per + i % per
        return place

    def to_partner(i):
        return remote(
            part.at[share(i) * 2 + (1 - b)], part_in.at[i], part_send.at[i], part_recv.at[i], partner
        )

    def to_owner(i, place):
        away = lax.rem(a - place + outer, outer) - 1
        return remote(
            part_in.at[i], part_far.at[away], sum_send.at[i], sum_recv.at[away], place * 2 + b
        )

    for j in range(width):
        from_lane = lax.rem(a // per + 1 + j, width)
        total = dot(x[from_lane].reshape(-1, x.shape[-1]), dv[...].reshape(-1, channels), TN)
        part[pl.ds(from_lane * per * 2, per * 2)] = total.astype(bf16).reshape(per * 2, rows_each, channels)
        for i in range(j * per, (j + 1) * per):
            to_partner(i).start()

    homeward(1)
    for low in range(0, devices, BATCH):
        query_terms(low)
    q[...] = (dq[...] * scale).astype(bf16)
    put_dq = pltpu.make_async_copy(q, dq_hbm, out_sem.at[1])
    put_dq.start()

    for i in range(outer):
        place = share(i)
        to_partner(i).wait_recv()
        both = part[place * 2 + b].astype(f32) + part_in[i].astype(f32)

        @pl.when(place == a)
        def _():
            dw[...] = both

        @pl.when(place != a)
        def _():
            part_in[i] = both.astype(bf16)
            to_owner(i, place).start()

    settle(1, dk)
    put_dk = pltpu.make_async_copy(dk, dk_hbm, out_sem.at[2])
    put_dk.start()

    for r in range(1, outer):
        remote(part_in.at[0], part_far.at[r - 1], sum_send.at[0], sum_recv.at[r - 1], partner).wait_recv()
        dw[...] += part_far[r - 1].astype(f32)
    put_dw = pltpu.make_async_copy(dw, dw_hbm, out_sem.at[3])
    put_dw.start()

    for ask in asks:
        ask.wait_send()
    for copy in x_far + [x_own] + x_onto:
        copy.wait_send()

    @pl.when(b == 0)
    def _():
        own().wait_send()

    for r in range(outer - 1):
        @pl.when((r <= a) & (a + 1 < outer))
        def _(r=r):
            chain(r).wait_send()

    @pl.loop(1, a + 1)
    def _(r):
        onto(r, b).wait_send()
        for kind in range(2):
            home(kind, r).wait_send()

    @pl.loop(1 - b, a + 1)
    def _(r):
        for kind in range(2):
            back(kind, r).wait_send()

    for i in range(outer):
        to_partner(i).wait_send()
        place = share(i)

        @pl.when(place != a)
        def _():
            to_owner(i, place).wait_send()

    for put in (put_dv, put_dq, put_dk, put_dw):
        put.wait()


def body(layer_input, queries, keys, values, outputs, d_out, log_sums, chosen):
    sequences, positions, channels = queries.shape
    features = layer_input.shape[2]
    heads = log_sums.shape[2]
    devices, width = lax.axis_size("kv"), lax.axis_size("tp")
    outer = devices // 2
    rows = width * features // devices
    batch = min(devices, BATCH)
    log_rows = (log_sums * LOG2E).transpose(0, 2, 1)
    dma, vmem = pltpu.SemaphoreType.DMA, pltpu.VMEM
    here, there = pl.BlockSpec(memory_space=pltpu.VMEM), pl.BlockSpec(memory_space=pl.ANY)
    shape = (sequences, positions, channels)
    tall = (sequences, positions // BLK, BLK, channels)
    block = (CAP, BLK, channels)
    d_queries, d_keys, d_values, d_weight = pl.pallas_call(
        functools.partial(kernel, devices, width, heads, (channels // heads) ** (-0.5)),
        in_specs=[there] * 6 + [here] * 2,
        out_specs=[there] * 4,
        out_shape=[
            jax.ShapeDtypeStruct(shape, bf16), jax.ShapeDtypeStruct(tall, bf16),
            jax.ShapeDtypeStruct(tall, bf16), jax.ShapeDtypeStruct((rows, channels), f32),
        ],
        scratch_shapes=[
            vmem((devices,) + chosen.shape, i32),
            vmem(shape, bf16), vmem(tall, bf16), vmem(tall, bf16), vmem(shape, bf16), vmem(shape, bf16),
            vmem((width, sequences, positions, features), bf16),
            vmem(shape, f32), vmem(tall, bf16), vmem(tall, bf16),
            vmem((sequences, heads, positions), f32),
            vmem((devices, 2) + block, bf16),
            vmem((heads, batch * CAP * BLK, positions), bf16),
            vmem((2, devices) + block, bf16),
            vmem((2, outer) + block, bf16),
            vmem((2, outer - 1) + block, bf16),
            vmem((devices, rows, channels), bf16),
            vmem((outer, rows, channels), bf16),
            vmem((outer - 1, rows, channels), bf16),
            vmem((rows, channels), f32),
            pltpu.SMEM((devices * CAP,), i32),
            dma((5, sequences)), dma, dma((4,)), dma((devices - 1,)), dma((devices - 1,)),
            dma((width - 1,)), dma((width - 1,)),
            dma, dma, dma((outer - 1,)), dma((outer - 1,)), dma((outer - 1,)), dma((outer - 1,)),
            dma((2, outer)), dma((2, outer)), dma((2, outer - 1)), dma((2, outer - 1)),
            dma((outer,)), dma((outer,)), dma((outer,)), dma((outer - 1,)),
        ],
        compiler_params=pltpu.CompilerParams(
            collective_id=0, has_side_effects=True, vmem_limit_bytes=67043328
        ),
        name="sparse_backward",
    )(
        layer_input, queries, keys.reshape(tall), values.reshape(tall), outputs, d_out, log_rows, chosen
    )
    return d_queries, d_keys.reshape(shape), d_values.reshape(shape), d_weight


def solution(mesh):
    split = P(None, "kv", "tp")
    return jax.shard_map(
        body,
        mesh=mesh,
        in_specs=(split,) * 7 + (P(None, "kv", None),),
        out_specs=(split, split, split, P("kv", "tp")),
        check_vma=False,
    )
```

```python
import functools

import jax
import jax.numpy as jnp
from jax import lax
from jax.experimental import pallas as pl
from jax.experimental.pallas import tpu as pltpu
from jax.sharding import PartitionSpec as P

BLK = 64
CAP = 2
LOG2E = 1.4426950408889634
HIDDEN = 1e30
GROUP = 4
BATCH = 8
PIECES = 2
NONE = 1 << 20

NT = (((1,), (1,)), ((), ()))
NN = (((1,), (0,)), ((), ()))
TN = (((0,), (0,)), ((), ()))
bf16, f32, i32 = jnp.bfloat16, jnp.float32, jnp.int32


def dot(a, b, dims):
    return lax.dot_general(a, b, dims, preferred_element_type=f32)


def peer(index, axis="kv"):
    return dict(device_id={axis: index}, device_id_type=pl.DeviceIdType.MESH)


def remote(source, target, send, recv, index, axis="kv"):
    return pltpu.make_async_remote_copy(source, target, send, recv, **peer(index, axis))


def probabilities(k, v, q, g, shift, delta, scale, diagonal):
    prob = jnp.exp2(dot(k, q, NT) * (scale * LOG2E) - shift)
    if diagonal:
        rows = lax.broadcasted_iota(i32, prob.shape, 0)
        cols = lax.broadcasted_iota(i32, prob.shape, 1)
        prob = jnp.where(rows <= cols, prob, 0.0)
    dscore = prob * (dot(v, g, NT) - delta)
    return prob.astype(bf16), dscore.astype(bf16)


def kernel(
    devices, width, heads, scale,
    x_hbm, q_hbm, k_hbm, v_hbm, o_hbm, g_hbm, log_ref, chosen_ref,
    dq_hbm, dk_hbm, dv_hbm, dw_hbm,
    every, q, k, v, o, g, x, dq, dk, dv, delta, pool, dscore, terms, back_in, back_far, part, part_in,
    part_far, pair_in, dw, table,
    load_sem, keep_sem, out_sem, every_send, every_recv, x_send, x_recv,
    own_send, own_recv, chain_send, chain_recv, pass_send, pass_recv,
    back_send, back_recv, home_send, home_recv, part_send, part_recv, sum_send, sum_recv, pair_recv,
):
    sequences, positions, channels = q.shape
    size = channels // heads
    blocks = positions // BLK
    outer = devices // 2
    me, lane = lax.axis_index("kv"), lax.axis_index("tp")
    a, b = me // 2, me % 2
    partner = a * 2 + (1 - b)
    core = lane // 2 * 2 + (1 - lane % 2)
    head = [slice(h * size, (h + 1) * size) for h in range(heads)]

    def load(j, s):
        source, target = ((k_hbm, k), (v_hbm, v), (q_hbm, q), (g_hbm, g), (o_hbm, o))[j]
        return pltpu.make_async_copy(source.at[s], target.at[s], load_sem.at[j, s])

    for j in range(5):
        for s in range(sequences):
            load(j, s).start()
    keep = pltpu.make_async_copy(x_hbm, x.at[lane], keep_sem)
    keep.start()

    barrier = pltpu.get_barrier_semaphore()
    for i in range(1, devices):
        pl.semaphore_signal(barrier, inc=1, **peer(lax.rem(me + i, devices)))
    for i in range(1, width):
        pl.semaphore_signal(barrier, inc=1, **peer(lax.rem(lane + i, width), "tp"))
    pl.semaphore_wait(barrier, devices + width - 2)

    asks = [
        remote(chosen_ref, every.at[me], every_send.at[i - 1], every_recv.at[i - 1], lax.rem(me + i, devices))
        for i in range(1, devices)
    ]
    for ask in asks:
        ask.start()
    x_far = [
        remote(x_hbm, x.at[lane], x_send.at[i - 1], x_recv.at[i - 1], lax.rem(lane + 2 * i, width), "tp")
        for i in range(1, width // 2)
    ]
    x_own = remote(x_hbm, x.at[lane], x_send.at[width - 2], x_recv.at[width - 2], core, "tp")
    x_onto = []
    for i in range(1, width // 2):
        origin = lax.rem(lane + width - 2 * i, width)
        at = width // 2 - 2 + i
        x_onto.append(remote(x.at[origin], x.at[origin], x_send.at[at], x_recv.at[at], core, "tp"))
    for copy in x_far + [x_own]:
        copy.start()
    every[pl.ds(me, 1)] = chosen_ref[...][None]

    seq_of = lax.broadcasted_iota(i32, (sequences,) + chosen_ref.shape[1:], 0)

    def named(owner):
        low = jnp.full(seq_of.shape, NONE, i32)
        for d in range(devices):
            local = every[d] - owner * blocks
            fits = (local >= 0) & (local < blocks) & (owner != d)
            low = jnp.where(fits, jnp.minimum(low, seq_of * blocks + local), low)
        first = jnp.min(low)
        rest = jnp.full(seq_of.shape, NONE, i32)
        for d in range(devices):
            local = every[d] - owner * blocks
            fits = (local >= 0) & (local < blocks) & (owner != d)
            value = seq_of * blocks + local
            rest = jnp.where(fits & (value != first), jnp.minimum(rest, value), rest)
        return first, jnp.min(rest)

    for ask in asks:
        ask.wait_recv()
    mine = named(me)
    for j in range(2):
        for s in range(sequences):
            load(j, s).wait()
    for n in range(CAP):
        block = jnp.where(mine[n] < NONE, mine[n], 0)
        s, place = lax.div(block, blocks), lax.rem(block, blocks)
        pool[me, 0, n] = k[s, place]
        pool[me, 1, n] = v[s, place]

    def own():
        return remote(pool.at[a * 2], pool.at[a * 2], own_send, own_recv, partner)

    def chain(r):
        at = pool.at[(a - r) * 2 + b]
        return remote(at, at, chain_send.at[r], chain_recv.at[r], (a + 1) * 2 + b)

    def arrive(r):
        at = pool.at[(a - r) * 2 + b]
        return remote(at, at, chain_send.at[r - 1], chain_recv.at[r - 1], partner)

    def onto(r, side):
        at = pool.at[(a - r) * 2 + side]
        return remote(at, at, pass_send.at[r - 1], pass_recv.at[r - 1], partner)

    @pl.when(b == 0)
    def _():
        own().start()

    @pl.when(a + 1 < outer)
    def _():
        chain(0).start()

    def relay(r):
        @pl.when(r <= a)
        def _():
            arrive(r).wait_recv()
            onto(r, b).start()

            @pl.when(a + 1 < outer)
            def _():
                chain(r).start()

    dscore[...] = jnp.zeros_like(dscore)

    @pl.loop(0, devices)
    def _(d):
        first, second = named(d)
        table[d * CAP] = jnp.where(d < me, first, NONE)
        table[d * CAP + 1] = jnp.where(d < me, second, NONE)

    spread = lax.broadcasted_iota(i32, (blocks, positions), 1) // BLK == lax.broadcasted_iota(
        i32, (blocks, positions), 0
    )

    def hide_row(asked, block):
        sees = jnp.max(jnp.where(asked == block, 1.0, 0.0), axis=1, keepdims=True)
        sees = jnp.where(spread, sees, 0.0)
        return (1.0 - jnp.sum(sees, axis=0, keepdims=True)) * HIDDEN

    chunk = GROUP * BLK

    @pl.loop(0, sequences)
    def _(s):
        for j in range(2, 5):
            load(j, s).wait()
        for r in range(1, outer):
            @pl.when(s == min(sequences - 1, 1 + (r - 1) * sequences // outer))
            def _(r=r):
                relay(r)
        asked = chosen_ref[s]
        hide = [hide_row(asked, me * blocks + i) for i in range(blocks)]
        for h in range(heads):
            product = g[s, :, head[h]].astype(f32) * o[s, :, head[h]].astype(f32)
            delta_row = jnp.sum(product.T, axis=0, keepdims=True)
            delta[s, h : h + 1] = delta_row
            log_row = log_ref[s, h : h + 1] * LOG2E
            for start in range(0, positions, chunk):
                keys, rest = slice(start // BLK, start // BLK + GROUP), slice(start, positions)
                shift = jnp.concatenate([
                    jnp.broadcast_to((log_row + hide[start // BLK + i])[:, rest], (BLK, positions - start))
                    for i in range(GROUP)
                ], axis=0)
                qq, gg = q[s, rest, head[h]], g[s, rest, head[h]]
                kk = k[s, keys, :, head[h]].reshape(chunk, size)
                vv = v[s, keys, :, head[h]].reshape(chunk, size)
                prob, dsc = probabilities(kk, vv, qq, gg, shift, delta_row[:, rest], scale, True)
                if start == 0:
                    dq[s, :, head[h]] = dot(dsc, kk, TN)
                else:
                    dq[s, rest, head[h]] += dot(dsc, kk, TN)
                tall = (GROUP, BLK, size)
                dk[s, keys, :, head[h]] = (dot(dsc, qq, NN) * scale).astype(bf16).reshape(tall)
                dv[s, keys, :, head[h]] = dot(prob, gg, NN).astype(bf16).reshape(tall)

    def far_terms(owner, at):
        for n in range(CAP):
            ident = table[owner * CAP + n]
            valid = ident < NONE
            ident = jnp.where(valid, ident, 0)
            s = lax.div(ident, blocks)
            block = jnp.where(valid, owner * blocks + lax.rem(ident, blocks), -2)
            hide = hide_row(chosen_ref[s], block)
            logs, deltas = log_ref[s] * LOG2E, delta[s]
            for h in range(heads):
                qq, gg = q[s, :, head[h]], g[s, :, head[h]]
                prob, dsc = probabilities(
                    pool[owner, 0, n, :, head[h]], pool[owner, 1, n, :, head[h]], qq, gg,
                    logs[h : h + 1] + hide, deltas[h : h + 1], scale, False,
                )
                dscore[h, pl.ds(pl.multiple_of((at * CAP + n) * BLK, BLK), BLK)] = dsc
                terms[0, owner, n, :, head[h]] = dot(prob, gg, NN).astype(bf16)
                terms[1, owner, n, :, head[h]] = (dot(dsc, qq, NN) * scale).astype(bf16)

    def back(kind, r):
        return remote(
            terms.at[kind, (a - r) * 2 + (1 - b)], back_in.at[kind, r],
            back_send.at[kind, r], back_recv.at[kind, r], partner,
        )

    def home(kind, r):
        return remote(
            back_in.at[kind, r], back_far.at[kind, r - 1],
            home_send.at[kind, r - 1], home_recv.at[kind, r - 1], (a - r) * 2 + b,
        )

    def query_terms(low):
        owners = min(devices - low, BATCH)
        for h in range(heads):
            masked = []
            for s in range(sequences):
                rows = []
                for i in range(owners):
                    for n in range(CAP):
                        ident = table[(low + i) * CAP + n]
                        rows.append(jnp.where(
                            lax.div(ident, blocks) == s, pool[low + i, 0, n, :, head[h]], 0.0
                        ).astype(bf16))
                masked.append(jnp.concatenate(rows, axis=0))
            more = dot(dscore[h], jnp.concatenate(masked, axis=1), TN)
            for s in range(sequences):
                dq[s, :, head[h]] += more[:, s * size : (s + 1) * size]

    @pl.when(b == 1)
    def _():
        own().wait_recv()
        far_terms(a * 2, (a * 2) % BATCH)
        back(0, 0).start()

    @pl.loop(1, a + 1)
    def _(r):
        direct, passed = (a - r) * 2 + b, (a - r) * 2 + (1 - b)
        onto(r, 1 - b).wait_recv()
        far_terms(passed, passed % BATCH)
        back(0, r).start()
        far_terms(direct, direct % BATCH)

    @pl.loop(1 - b, a + 1)
    def _(r):
        back(1, r).start()

    def homeward(kind):
        @pl.loop(1, a + 1)
        def _(r):
            back(kind, r).wait_recv()
            both = terms[kind, (a - r) * 2 + b].astype(f32) + back_in[kind, r].astype(f32)
            back_in[kind, r] = both.astype(bf16)
            home(kind, r).start()

    def settle(kind, rows):
        @pl.when(b == 0)
        def _():
            back(kind, 0).wait_recv()

        @pl.when(b == 1)
        def _():
            back_in[kind, 0] = jnp.zeros(back_in.shape[2:], bf16)

        summed = back_in[kind, 0].astype(f32)
        for r in range(1, outer):
            @pl.when(a + r < outer)
            def _(r=r):
                home(kind, r).wait_recv()

            @pl.when(a + r >= outer)
            def _(r=r):
                back_far[kind, r - 1] = jnp.zeros(back_far.shape[2:], bf16)

            summed += back_far[kind, r - 1].astype(f32)
        fresh = []
        for n in range(CAP):
            block = jnp.where(mine[n] < NONE, mine[n], 0)
            s, place = lax.div(block, blocks), lax.rem(block, blocks)
            fresh.append((rows[s, place].astype(f32) + summed[n]).astype(bf16))
        for s in range(sequences):
            for i in range(blocks):
                value = rows[s, i]
                for n in range(CAP):
                    value = jnp.where(mine[n] == s * blocks + i, fresh[n], value)
                rows[s, i] = value

    homeward(0)
    settle(0, dv)
    put_dv = pltpu.make_async_copy(dv, dv_hbm, out_sem.at[0])
    put_dv.start()

    per = outer // width
    rows_each = dw.shape[1]

    def from_lane(j):
        return lax.rem((lane if j % 2 == 0 else core) + width - j // 2 * 2, width)

    def share(t):
        i = t // PIECES
        return from_lane(i // per) * per + i % per

    def to_partner(t):
        source = (share(t) * 2 + (1 - b)) * PIECES + t % PIECES
        return remote(part.at[source], part_in.at[t], part_send.at[t], part_recv.at[t], partner)

    def to_owner(t, place):
        at = (lax.rem(a - place + outer, outer) - 1) * PIECES + t % PIECES
        return remote(part_in.at[t], part_far.at[at], sum_send.at[t], sum_recv.at[at], place * 2 + b)

    half = outer // 2
    paired = outer == 4
    inner = (a == half - 1) | (a == half)

    def to_inner(t, chip):
        return remote(part_in.at[t], pair_in.at[t], sum_send.at[t], pair_recv.at[t], chip)

    for j in range(width):
        if j == 0:
            keep.wait()
        elif j == 1:
            x_own.wait_recv()
        elif j % 2 == 0:
            x_far[j // 2 - 1].wait_recv()
            x_onto[j // 2 - 1].start()
        else:
            x_onto[j // 2 - 1].wait_recv()
        total = dot(x[from_lane(j)].reshape(-1, x.shape[-1]), dv[...].reshape(-1, channels), TN)
        many = per * 2 * PIECES
        part[pl.ds(from_lane(j) * many, many)] = total.astype(bf16).reshape(many, rows_each, channels)
        for t in range(j * per * PIECES, (j + 1) * per * PIECES):
            to_partner(t).start()

    homeward(1)
    for t in range(outer * PIECES):
        place = share(t)
        to_partner(t).wait_recv()
        both = part[(place * 2 + b) * PIECES + t % PIECES].astype(f32) + part_in[t].astype(f32)
        crossing = ((place < half) != (a < half)) & paired

        @pl.when(place == a)
        def _():
            dw[t % PIECES] = both

        @pl.when((place != a) & jnp.logical_not(crossing))
        def _():
            part_in[t] = both.astype(bf16)
            to_owner(t, place).start()

        if paired:
            @pl.when(crossing & inner)
            def _():
                to_inner(t, partner).wait_recv()
                part_in[t] = (both + pair_in[t].astype(f32)).astype(bf16)
                to_owner(t, place).start()

            @pl.when(crossing & jnp.logical_not(inner))
            def _():
                part_in[t] = both.astype(bf16)
                to_inner(t, jnp.where(a < half, half - 1, half) * 2 + b).start()

    for low in range(0, devices, BATCH):
        query_terms(low)
    q[...] = (dq[...] * scale).astype(bf16)
    put_dq = pltpu.make_async_copy(q, dq_hbm, out_sem.at[1])
    put_dq.start()

    settle(1, dk)
    put_dk = pltpu.make_async_copy(dk, dk_hbm, out_sem.at[2])
    put_dk.start()

    for c in range(PIECES):
        for r in range(1, outer):
            source = lax.rem(a + r, outer)
            near = (source < half) == (a < half)
            at = (r - 1) * PIECES + c

            @pl.when(near | (source == half - 1) | (source == half) | (not paired))
            def _(at=at, c=c):
                remote(part_in.at[0], part_far.at[at], sum_send.at[0], sum_recv.at[at], partner).wait_recv()
                dw[c] += part_far[at].astype(f32)
    put_dw = pltpu.make_async_copy(dw, dw_hbm, out_sem.at[3])
    put_dw.start()

    for ask in asks:
        ask.wait_send()
    for copy in x_far + [x_own] + x_onto:
        copy.wait_send()

    @pl.when(b == 0)
    def _():
        own().wait_send()

    for r in range(outer - 1):
        @pl.when((r <= a) & (a + 1 < outer))
        def _(r=r):
            chain(r).wait_send()

    @pl.loop(1, a + 1)
    def _(r):
        onto(r, b).wait_send()
        for kind in range(2):
            home(kind, r).wait_send()

    @pl.loop(1 - b, a + 1)
    def _(r):
        for kind in range(2):
            back(kind, r).wait_send()

    for t in range(outer * PIECES):
        to_partner(t).wait_send()
        place = share(t)

        @pl.when(place != a)
        def _():
            to_inner(t, partner).wait_send()

    for put in (put_dv, put_dq, put_dk, put_dw):
        put.wait()


def body(layer_input, queries, keys, values, outputs, d_out, log_sums, chosen):
    sequences, positions, channels = queries.shape
    features = layer_input.shape[2]
    heads = log_sums.shape[2]
    devices, width = lax.axis_size("kv"), lax.axis_size("tp")
    outer = devices // 2
    rows = width * features // devices
    batch = min(devices, BATCH)
    log_rows = log_sums.transpose(0, 2, 1)
    dma, vmem = pltpu.SemaphoreType.DMA, pltpu.VMEM
    here, there = pl.BlockSpec(memory_space=pltpu.VMEM), pl.BlockSpec(memory_space=pl.ANY)
    shape = (sequences, positions, channels)
    tall = (sequences, positions // BLK, BLK, channels)
    block = (CAP, BLK, channels)
    piece = (rows // PIECES, channels)
    d_queries, d_keys, d_values, d_weight = pl.pallas_call(
        functools.partial(kernel, devices, width, heads, (channels // heads) ** (-0.5)),
        in_specs=[there] * 6 + [here] * 2,
        out_specs=[there] * 4,
        out_shape=[
            jax.ShapeDtypeStruct(shape, bf16), jax.ShapeDtypeStruct(tall, bf16),
            jax.ShapeDtypeStruct(tall, bf16), jax.ShapeDtypeStruct((PIECES,) + piece, f32),
        ],
        scratch_shapes=[
            vmem((devices,) + chosen.shape, i32),
            vmem(shape, bf16), vmem(tall, bf16), vmem(tall, bf16), vmem(shape, bf16), vmem(shape, bf16),
            vmem((width, sequences, positions, features), bf16),
            vmem(shape, f32), vmem(tall, bf16), vmem(tall, bf16),
            vmem((sequences, heads, positions), f32),
            vmem((devices, 2) + block, bf16),
            vmem((heads, batch * CAP * BLK, positions), bf16),
            vmem((2, devices) + block, bf16),
            vmem((2, outer) + block, bf16),
            vmem((2, outer - 1) + block, bf16),
            vmem((devices * PIECES,) + piece, bf16),
            vmem((outer * PIECES,) + piece, bf16),
            vmem(((outer - 1) * PIECES,) + piece, bf16),
            vmem((outer * PIECES if outer == 4 else 1,) + piece, bf16),
            vmem((PIECES,) + piece, f32),
            pltpu.SMEM((devices * CAP,), i32),
            dma((5, sequences)), dma, dma((4,)), dma((devices - 1,)), dma((devices - 1,)),
            dma((width - 1,)), dma((width - 1,)),
            dma, dma, dma((outer - 1,)), dma((outer - 1,)), dma((outer - 1,)), dma((outer - 1,)),
            dma((2, outer)), dma((2, outer)), dma((2, outer - 1)), dma((2, outer - 1)),
            *[dma((outer * PIECES,))] * 3, dma(((outer - 1) * PIECES,)), dma((outer * PIECES,)),
        ],
        compiler_params=pltpu.CompilerParams(
            collective_id=0, has_side_effects=True, vmem_limit_bytes=min(67043328, (34 * 2 + 3 * devices) * 2**19)
        ),
        name="sparse_backward",
    )(
        layer_input, queries, keys.reshape(tall), values.reshape(tall), outputs, d_out, log_rows, chosen
    )
    return d_queries, d_keys.reshape(shape), d_values.reshape(shape), d_weight.reshape(rows, channels)


def solution(mesh):
    split = P(None, "kv", "tp")
    return jax.shard_map(
        body,
        mesh=mesh,
        in_specs=(split,) * 7 + (P(None, "kv", None),),
        out_specs=(split, split, split, P("kv", "tp")),
        check_vma=False,
    )
```
